32 devices in a mesh: fs: 4 (over z), rep: 2 (over y), tp: 4 (over x, core).
Axes of the slice: x: 2, y: 2, z: 4, core: 2. Of those that a mesh axis runs over, the one named last changes fastest.
Arguments:
- saved_hidden: bfloat16 [7168, 2048], P(('fs', 'rep')), may hold values from -12 to 12
- grad_value: bfloat16 [7168, 1024], P(('fs', 'rep'), 'tp'), may hold values from -12 to 12
- saved_mixed: bfloat16 [7168, 1024], P(('fs', 'rep'), 'tp'), may hold values from -12 to 12
- grad_output: bfloat16 [7168, 2048], P(('fs', 'rep')), may hold values from -12 to 12
- basis_value: bfloat16 [2048, 128], replicated, may hold values from -0.5 to 0.5
- basis_output: bfloat16 [2048, 128], replicated, may hold values from -0.5 to 0.5
- weight_value: float32 [2048, 1024], P('fs', 'tp'), may hold values from -0.125 to 0.125
- weight_output: float32 [1024, 2048], P('tp', 'fs'), may hold values from -0.1875 to 0.1875
- first_value: float32 [128, 1024], P('fs', 'tp'), may hold values from -4 to 4
- second_value: float32 [128, 1024], P('fs', 'tp'), may hold values from 0.05 to 0.5
- first_output: float32 [128, 1024], P('fs', 'tp'), may hold values from -4 to 4
- second_output: float32 [128, 1024], P('fs', 'tp'), may hold values from 0.05 to 0.5
Outputs:
- step_value: float32 [2048, 1024], P('fs', 'tp')
- step_output: float32 [1024, 2048], P('tp', 'fs')
- new_weight_value: float32 [2048, 1024], P('fs', 'tp')
- new_weight_output: float32 [1024, 2048], P('tp', 'fs')
- copy_value: bfloat16 [2048, 1024], P(None, 'tp')
- copy_output: bfloat16 [1024, 2048], P('tp')
- new_first_value: float32 [128, 1024], P('fs', 'tp')
- new_second_value: float32 [128, 1024], P('fs', 'tp')
- new_first_output: float32 [128, 1024], P('fs', 'tp')
- new_second_output: float32 [128, 1024], P('fs', 'tp')
The draws below stay inside these ranges and needn't reach their ends.
All inputs are finite; a program needn't handle non-finite values.
Results may differ from the reference program's by a relative error of at most 0.0045.
Values may be sent and summed in bfloat16 or wider, within the bound.
A program may use at most 64 MiB of HBM per device.

```python
import math
import jax
import jax.numpy as jnp
from jax import lax

D = 2048
AW = 1024
RANK = 128
TOKENS = 7168


def field_values(key, row_total, col_total, rising_columns):
    key_noise = jax.random.fold_in(key, 0)
    length = col_total if rising_columns else row_total
    position = jnp.arange(length, dtype=jnp.float32) / max(length - 1, 1)
    noise_field = jnp.clip(jax.random.normal(key_noise, (row_total, col_total), jnp.float32), -4.0, 4.0)
    scales = jnp.exp(math.log(3.0) * position)
    if rising_columns:
        return noise_field * scales[None, :]
    return noise_field * scales[:, None]


def draw_saved_hidden(key, part):
    return field_values(jax.random.fold_in(key, 11), TOKENS, D, False).astype(jnp.bfloat16)


def draw_grad_value(key, part):
    return field_values(jax.random.fold_in(key, 23), TOKENS, AW, True).astype(jnp.bfloat16)


def draw_saved_mixed(key, part):
    return field_values(jax.random.fold_in(key, 37), TOKENS, AW, True).astype(jnp.bfloat16)


def draw_grad_output(key, part):
    return field_values(jax.random.fold_in(key, 41), TOKENS, D, False).astype(jnp.bfloat16)


def steps_of(own_key, extent, cuts, smallest, top_value):
    loudness = 1.0
    for axis_at, shards_of in cuts:
        heights = jax.random.uniform(jax.random.fold_in(jax.random.fold_in(own_key, 6), axis_at), (shards_of,), jnp.float32, smallest / len(cuts), top_value / len(cuts))
        loudness = loudness * jnp.repeat(jnp.exp(heights), extent[axis_at] // shards_of).reshape((-1,) + (1,) * (len(extent) - 1 - axis_at))
    return loudness


def centred(rng, dims, scale, most, cuts=(), held_as=jnp.bfloat16):
    result = scale * jax.random.normal(rng, dims, jnp.float32)
    if cuts:
        result = result * steps_of(rng, dims, cuts, -0.22, 0.18)
    return jnp.clip(result, -most, most).astype(held_as)


def setup_inputs(seed: int = 0) -> dict:
    streams_of = jax.random.split(jax.random.key(seed), 13)
    return {
        "saved_hidden": draw_saved_hidden(jax.random.fold_in(streams_of[12], 71), 0),
        "grad_value": draw_grad_value(jax.random.fold_in(streams_of[12], 71), 0),
        "saved_mixed": draw_saved_mixed(jax.random.fold_in(streams_of[12], 71), 0),
        "grad_output": draw_grad_output(jax.random.fold_in(streams_of[12], 71), 0),
        "basis_value": centred(streams_of[4], (D, RANK), RANK ** -0.5, 0.5),
        "basis_output": centred(streams_of[5], (D, RANK), RANK ** -0.5, 0.5),
        "weight_value": centred(streams_of[6], (D, AW), D ** -0.5, 0.125, ((0, 4), (1, 4)), jnp.float32),
        "weight_output": centred(streams_of[7], (AW, D), AW ** -0.5, 0.1875, ((0, 4), (1, 4)), jnp.float32),
        "first_value": centred(streams_of[8], (RANK, AW), 1.0, 4.0, ((0, 4), (1, 4)), jnp.float32),
        "second_value": jnp.clip(jnp.exp(math.log(0.5) - 2.3025851 * jax.random.uniform(streams_of[9], (RANK, AW), jnp.float32) ** steps_of(streams_of[9], (RANK, AW), ((0, 4), (1, 4)), -0.2, 0.2)), 0.05, 0.5),
        "first_output": centred(streams_of[10], (RANK, AW), 1.0, 4.0, ((0, 4), (1, 4)), jnp.float32),
        "second_output": jnp.clip(jnp.exp(math.log(0.5) - 2.3025851 * jax.random.uniform(streams_of[11], (RANK, AW), jnp.float32) ** steps_of(streams_of[11], (RANK, AW), ((0, 4), (1, 4)), -0.2, 0.2)), 0.05, 0.5),
    }


first_decay = 0.8
second_decay = 0.9
learning_rate = 0.02
norm_epsilon = 1e-06

def project(basis, gradient):
    return jnp.dot(basis.astype(jnp.float32).T, gradient, precision=lax.Precision.HIGHEST)

def moments(projected, first_old, second_old, clip_factor):
    scaled = clip_factor * projected
    first_new = first_decay * first_old + (1.0 - first_decay) * scaled
    second_new = second_decay * second_old + (1.0 - second_decay) * scaled * scaled
    return (first_new, second_new, first_new / jnp.sqrt(second_new))

def reference(saved_hidden, grad_value, saved_mixed, grad_output, basis_value, basis_output, weight_value, weight_output, first_value, second_value, first_output, second_output):
    gradient_value = jnp.dot(saved_hidden.T, grad_value, preferred_element_type=jnp.float32)
    gradient_output = jnp.dot(grad_output.T, saved_mixed, preferred_element_type=jnp.float32)
    projected_value = project(basis_value, gradient_value)
    projected_output = project(basis_output, gradient_output)
    squares = jnp.sum(projected_value * projected_value) + jnp.sum(projected_output * projected_output)
    mean_square = squares / (2 * RANK * AW)
    clip_factor = jnp.minimum(1.0, 1.0 / jnp.sqrt(mean_square + norm_epsilon))
    first_new_value, second_new_value, direction_value = moments(projected_value, first_value, second_value, clip_factor)
    first_new_output, second_new_output, direction_output = moments(projected_output, first_output, second_output, clip_factor)
    step_value = jnp.dot(basis_value.astype(jnp.float32), direction_value, precision=lax.Precision.HIGHEST)
    step_output = jnp.dot(basis_output.astype(jnp.float32), direction_output, precision=lax.Precision.HIGHEST).T
    new_weight_value = weight_value - learning_rate * step_value
    new_weight_output = weight_output - learning_rate * step_output
    return (step_value, step_output, new_weight_value, new_weight_output, new_weight_value.astype(jnp.bfloat16), new_weight_output.astype(jnp.bfloat16), first_new_value, second_new_value, first_new_output, second_new_output)
```

```python
import functools
import jax
import jax.numpy as jnp
from jax import lax
from jax.experimental import pallas as pl
from jax.experimental.pallas import tpu as pltpu
from jax.sharding import PartitionSpec as P

AW = 1024
RANK = 128


first_decay = 0.8
second_decay = 0.9
learning_rate = 0.02
norm_epsilon = 1e-06
contract_leading = (((0,), (0,)), ((), ()))


def moments(projected, first_old, second_old, clip_factor):
    scaled = clip_factor * projected
    first_new = first_decay * first_old + (1.0 - first_decay) * scaled
    second_new = second_decay * second_old + (1.0 - second_decay) * scaled * scaled
    return (first_new, second_new, first_new / jnp.sqrt(second_new))


def split_product(reduced, other):
    upper = reduced.astype(jnp.bfloat16)
    lower = (reduced - upper.astype(jnp.float32)).astype(jnp.bfloat16)
    rank_count = reduced.shape[1]
    stacked = jnp.concatenate([upper, lower], axis=1)
    both = lax.dot_general(stacked, other, contract_leading, preferred_element_type=jnp.float32)
    return both[:rank_count] + both[rank_count:]


def local(
    saved_hidden,
    grad_value,
    saved_mixed,
    grad_output,
    basis_value,
    basis_output,
    weight_value,
    weight_output,
    first_value,
    second_value,
    first_output,
    second_output,
):
    row_count = weight_value.shape[0]
    moment_count = first_value.shape[0]
    fs_index = lax.axis_index("fs")
    row_first = fs_index * row_count
    moment_first = fs_index * moment_count
    value_basis_rows = lax.dynamic_slice_in_dim(basis_value, row_first, row_count, 0).astype(
        jnp.float32
    )
    output_basis_rows = lax.dynamic_slice_in_dim(basis_output, row_first, row_count, 0).astype(
        jnp.float32
    )
    reduced_hidden = jnp.dot(saved_hidden, basis_value, preferred_element_type=jnp.float32)
    reduced_output = jnp.dot(grad_output, basis_output, preferred_element_type=jnp.float32)
    part_value = split_product(reduced_hidden, grad_value)
    part_output = split_product(reduced_output, saved_mixed)
    projected_value, projected_output = lax.psum((part_value, part_output), ("fs", "rep"))
    local_squares = jnp.sum(projected_value * projected_value) + jnp.sum(
        projected_output * projected_output
    )
    total_squares = lax.psum(local_squares, "tp")
    mean_square = total_squares / (2 * RANK * AW)
    clip_factor = jnp.minimum(1.0, 1.0 / jnp.sqrt(mean_square + norm_epsilon))
    value_slice = lax.dynamic_slice_in_dim(projected_value, moment_first, moment_count, 0)
    output_slice = lax.dynamic_slice_in_dim(projected_output, moment_first, moment_count, 0)
    new_first_value, new_second_value, value_direction_rows = moments(
        value_slice, first_value, second_value, clip_factor
    )
    new_first_output, new_second_output, output_direction_rows = moments(
        output_slice, first_output, second_output, clip_factor
    )
    direction_value, direction_output = (
        lax.all_gather(value_direction_rows, "fs", axis=0, tiled=True),
        lax.all_gather(output_direction_rows, "fs", axis=0, tiled=True),
    )
    step_value = jnp.dot(value_basis_rows, direction_value, precision=lax.Precision.HIGHEST)
    step_output = jnp.dot(output_basis_rows, direction_output, precision=lax.Precision.HIGHEST).T
    new_weight_value = weight_value - learning_rate * step_value
    new_weight_output = weight_output - learning_rate * step_output
    copy_value, copy_output = (
        lax.all_gather(new_weight_value.astype(jnp.bfloat16), "fs", axis=0, tiled=True),
        lax.all_gather(new_weight_output.astype(jnp.bfloat16), "fs", axis=1, tiled=True),
    )
    return (
        step_value,
        step_output,
        new_weight_value,
        new_weight_output,
        copy_value,
        copy_output,
        new_first_value,
        new_second_value,
        new_first_output,
        new_second_output,
    )


MESH = pl.DeviceIdType.MESH


def remote(src, dst, send, recv, **where):
    return pltpu.make_async_remote_copy(
        src_ref=src, dst_ref=dst, send_sem=send, recv_sem=recv, device_id=where, device_id_type=MESH
    )


def exchange(
    fs_count, rep_count, tp_count,
    hidden, grad_value, mixed, grad_output, basis_value, basis_output, weight_value, weight_output,
    first_value, second_value, first_output, second_output,
    direction, owned, clip, all_value, all_output,
    tokens_in, thin_in, basis_in, value_in, output_in, moment_in,
    part, landed, squares_tp, squares_group,
    load_sem, near_send, near_recv, side_send, side_recv, part_send, part_recv,
    tp_send, tp_recv, group_send, group_recv, owned_send, owned_recv, turn_send, turn_recv,
):
    group = fs_count * rep_count
    fs, rep, tp = lax.axis_index("fs"), lax.axis_index("rep"), lax.axis_index("tp")
    me = fs * rep_count + rep
    tokens = hidden.shape[0]
    rows = part.shape[2]
    width = part.shape[3]
    half = tokens // 2

    loads = []

    def load(source, target):
        copy = pltpu.make_async_copy(source, target, load_sem.at[len(loads)])
        copy.start()
        loads.append(copy)
        return copy

    weight_loads = [load(weight_value, value_in), load(weight_output, output_in)]
    stream_loads = []
    for a, (big, thin, basis) in enumerate(
        ((hidden, grad_value, basis_value), (grad_output, mixed, basis_output))
    ):
        first = load(basis, basis_in.at[a])
        second = load(thin, thin_in.at[a])
        blocks = [
            load(big.at[pl.ds(c * half, half)], tokens_in.at[a, pl.ds(c * half, half)])
            for c in range(2)
        ]
        stream_loads.append((first, second, blocks))
    moment_loads = [
        load(source.at[pl.ds(pl.multiple_of(rep * rows, rows), rows)], moment_in.at[i])
        for i, source in enumerate((first_value, first_output, second_value, second_output))
    ]

    def member(k):
        other = lax.rem(me + k, group)
        return {"fs": other // rep_count, "rep": lax.rem(other, rep_count)}

    barrier = pltpu.get_barrier_semaphore()
    for k in range(1, group):
        pl.semaphore_signal(barrier, inc=1, device_id=member(k), device_id_type=MESH)
    for k in range(1, tp_count):
        pl.semaphore_signal(
            barrier, inc=1, device_id={"tp": lax.rem(tp + k, tp_count)}, device_id_type=MESH
        )
    for copy in weight_loads:
        copy.wait()
    all_value[fs] = value_in[...].astype(jnp.bfloat16)
    all_output[fs] = output_in[...].astype(jnp.bfloat16)
    pl.semaphore_wait(barrier, group - 1 + tp_count - 1)

    share_value = value_in.shape[0] // rep_count
    share_output = output_in.shape[0] // rep_count
    shares = (
        (all_value, pl.ds(pl.multiple_of(rep * share_value, share_value), share_value)),
        (all_output, pl.ds(pl.multiple_of(rep * share_output, share_output), share_output)),
    )
    sent = []

    def send(copy):
        copy.start()
        sent.append(copy)
        return copy

    far = {}

    def send_weights(k):
        far[k] = [
            send(remote(
                buffer.at[fs, rows_here], buffer.at[fs, rows_here],
                near_send.at[a, k - 1], near_recv.at[a, k - 1], fs=lax.rem(fs + k, fs_count),
            ))
            for a, (buffer, rows_here) in enumerate(shares)
        ]

    side = []

    def pass_weights(k):
        origin = lax.rem(fs + fs_count - k, fs_count)
        for a, (buffer, rows_here) in enumerate(shares):
            far[k][a].wait_recv()
            for j in range(1, rep_count):
                side.append(send(remote(
                    buffer.at[origin, rows_here], buffer.at[origin, rows_here],
                    side_send.at[a, k - 1, j - 1], side_recv.at[a, k - 1, j - 1],
                    rep=lax.rem(rep + j, rep_count),
                )))

    near = sorted({1, fs_count - 1})
    for k in near:
        send_weights(k)

    parts = []
    for a in range(2):
        first, second, blocks = stream_loads[a]
        first.wait()
        second.wait()
        total = None
        for c in range(2):
            blocks[c].wait()
            reduced = jnp.dot(
                tokens_in[a, pl.ds(c * half, half)], basis_in[a], preferred_element_type=jnp.float32
            )
            product = split_product(reduced, thin_in[a, pl.ds(c * half, half)])
            total = product if total is None else total + product
        part[a] = total.reshape(group, rows, width)
        for k in range(1, group):
            other = lax.rem(me + k, group)
            parts.append(send(remote(
                part.at[a, other], landed.at[a, k - 1],
                part_send.at[a, k - 1], part_recv.at[a, k - 1], **member(k),
            )))

    for k in range(2, fs_count - 1):
        send_weights(k)
    for k in near:
        pass_weights(k)

    for copy in parts:
        copy.wait_recv()
    squares = jnp.zeros((rows, width), jnp.float32)
    for a in range(2):
        summed = part[a, me]
        for k in range(group - 1):
            summed = summed + landed[a, k]
        owned[rep, a] = summed
        squares = squares + summed * summed
    squares_tp[0] = jnp.full(squares_tp.shape[1:], jnp.sum(squares), jnp.float32)
    tp_copies = [
        send(remote(
            squares_tp.at[0], squares_tp.at[k], tp_send.at[k - 1], tp_recv.at[k - 1],
            tp=lax.rem(tp + k, tp_count),
        ))
        for k in range(1, tp_count)
    ]
    owned_copies = [
        send(remote(
            owned.at[rep], owned.at[rep], owned_send.at[j - 1], owned_recv.at[j - 1],
            rep=lax.rem(rep + j, rep_count),
        ))
        for j in range(1, rep_count)
    ]
    for copy in tp_copies:
        copy.wait_recv()
    squares_group[me] = jnp.sum(squares_tp[...], axis=0)
    group_copies = [
        send(remote(
            squares_group.at[me], squares_group.at[me], group_send.at[k - 1], group_recv.at[k - 1],
            **member(k),
        ))
        for k in range(1, group)
    ]
    for copy in moment_loads:
        copy.wait()
    for copy in group_copies:
        copy.wait_recv()
    mean_square = jnp.sum(squares_group[...], axis=0) / (2 * RANK * AW)
    factor = jnp.minimum(1.0, 1.0 / jnp.sqrt(mean_square + norm_epsilon))
    clip[...] = factor
    scale = factor[:1, :1]
    for a in range(2):
        _, _, turned = moments(owned[rep, a], moment_in[a], moment_in[2 + a], scale)
        direction[me, a] = turned.astype(jnp.bfloat16)
    turn_copies = [
        send(remote(
            direction.at[me], direction.at[me], turn_send.at[k - 1], turn_recv.at[k - 1], **member(k)
        ))
        for k in range(1, group)
    ]
    for k in range(2, fs_count - 1):
        pass_weights(k)
    for copy in owned_copies + turn_copies + side:
        copy.wait_recv()
    for copy in sent:
        copy.wait_send()


def finish(
    direction, owned, clip, all_value, all_output, basis_value, basis_output,
    weight_value, weight_output, first_value, second_value, first_output, second_output,
    step_value, step_output, new_weight_value, new_weight_output, copy_value, copy_output,
    new_first_value, new_second_value, new_first_output, new_second_output,
):
    fs = lax.axis_index("fs")
    count = weight_value.shape[0]
    width = weight_value.shape[1]
    scale = clip[:1, :1]
    outputs = ((new_first_value, new_second_value), (new_first_output, new_second_output))
    for a, (first, second) in enumerate(
        ((first_value, second_value), (first_output, second_output))
    ):
        projected = owned[:, a].reshape(first.shape)
        new_first, new_second, _ = moments(projected, first[...], second[...], scale)
        outputs[a][0][...] = new_first
        outputs[a][1][...] = new_second
    turn_value = direction[:, 0].reshape(RANK, width)
    turn_output = direction[:, 1].reshape(RANK, width).astype(jnp.float32).T.astype(jnp.bfloat16)
    across = (((1,), (1,)), ((), ()))

    def value_step(rows_here):
        return jnp.dot(basis_value[rows_here], turn_value, preferred_element_type=jnp.float32)

    def output_step(rows_here):
        return lax.dot_general(
            turn_output, basis_output[rows_here], across, preferred_element_type=jnp.float32
        )

    mine = pl.ds(pl.multiple_of(fs * count, count), count)
    step = value_step(mine)
    step_value[...] = step
    new_weight_value[...] = weight_value[...] - learning_rate * step
    step = output_step(mine)
    step_output[...] = step
    new_weight_output[...] = weight_output[...] - learning_rate * step
    for f in range(all_value.shape[0]):
        here = pl.ds(f * count, count)
        copy_value[here] = (
            all_value[f].astype(jnp.float32) - learning_rate * value_step(here)
        ).astype(jnp.bfloat16)
        copy_output[:, here] = (
            all_output[f].astype(jnp.float32) - learning_rate * output_step(here)
        ).astype(jnp.bfloat16)


def kernels(
    fs_count, rep_count, tp_count,
    saved_hidden, grad_value, saved_mixed, grad_output, basis_value, basis_output,
    weight_value, weight_output, first_value, second_value, first_output, second_output,
):
    group = fs_count * rep_count
    tokens, model = saved_hidden.shape
    count, width = weight_value.shape
    rank = basis_value.shape[1]
    rows = rank // group
    f32, bf16 = jnp.float32, jnp.bfloat16
    shape = jax.ShapeDtypeStruct
    dma = pltpu.SemaphoreType.DMA
    anywhere = pl.BlockSpec(memory_space=pl.ANY)
    in_vmem = pl.BlockSpec(memory_space=pltpu.VMEM)
    direction, owned, clip, all_value, all_output = pl.pallas_call(
        functools.partial(exchange, fs_count, rep_count, tp_count),
        out_shape=(
            shape((group, 2, rows, width), bf16),
            shape((rep_count, 2, rows, width), f32),
            shape((8, 128), f32),
            shape((fs_count, count, width), bf16),
            shape((fs_count, width, count), bf16),
        ),
        in_specs=[anywhere] * 12,
        out_specs=(in_vmem,) * 5,
        scratch_shapes=[
            pltpu.VMEM((2, tokens, model), bf16),
            pltpu.VMEM((2, tokens, width), bf16),
            pltpu.VMEM((2, model, rank), bf16),
            pltpu.VMEM((count, width), f32),
            pltpu.VMEM((width, count), f32),
            pltpu.VMEM((4, rows, width), f32),
            pltpu.VMEM((2, group, rows, width), f32),
            pltpu.VMEM((2, group - 1, rows, width), f32),
            pltpu.VMEM((tp_count, 8, 128), f32),
            pltpu.VMEM((group, 8, 128), f32),
            dma((14,)),
            dma((2, fs_count - 1)), dma((2, fs_count - 1)),
            dma((2, fs_count - 1, rep_count - 1)), dma((2, fs_count - 1, rep_count - 1)),
            dma((2, group - 1)), dma((2, group - 1)),
            dma((tp_count - 1,)), dma((tp_count - 1,)),
            dma((group - 1,)), dma((group - 1,)),
            dma((rep_count - 1,)), dma((rep_count - 1,)),
            dma((group - 1,)), dma((group - 1,)),
        ],
        compiler_params=pltpu.CompilerParams(
            collective_id=0, has_side_effects=True, vmem_limit_bytes=32 * 1024 * 1024
        ),
        name="exchange",
    )(
        saved_hidden, grad_value, saved_mixed, grad_output, basis_value, basis_output,
        weight_value, weight_output, first_value, second_value, first_output, second_output,
    )
    moment = shape(first_value.shape, f32)
    return pl.pallas_call(
        finish,
        out_shape=(
            shape((count, width), f32), shape((width, count), f32),
            shape((count, width), f32), shape((width, count), f32),
            shape((model, width), bf16), shape((width, model), bf16),
            moment, moment, moment, moment,
        ),
        in_specs=[in_vmem] * 13,
        out_specs=(in_vmem,) * 10,
        compiler_params=pltpu.CompilerParams(vmem_limit_bytes=32 * 1024 * 1024),
        name="finish",
    )(
        direction, owned, clip, all_value, all_output, basis_value, basis_output,
        weight_value, weight_output, first_value, second_value, first_output, second_output,
    )


def solution(mesh):
    fs_count, rep_count, tp_count = mesh.shape["fs"], mesh.shape["rep"], mesh.shape["tp"]
    whole_tiles = RANK % (16 * fs_count * rep_count) == 0
    body = functools.partial(kernels, fs_count, rep_count, tp_count) if whole_tiles else local
    return jax.shard_map(
        body,
        mesh=mesh,
        in_specs=(
            P(("fs", "rep"), None),
            P(("fs", "rep"), "tp"),
            P(("fs", "rep"), "tp"),
            P(("fs", "rep"), None),
            P(),
            P(),
            P("fs", "tp"),
            P("tp", "fs"),
            P("fs", "tp"),
            P("fs", "tp"),
            P("fs", "tp"),
            P("fs", "tp"),
        ),
        out_specs=(
            P("fs", "tp"),
            P("tp", "fs"),
            P("fs", "tp"),
            P("tp", "fs"),
            P(None, "tp"),
            P("tp", None),
            P("fs", "tp"),
            P("fs", "tp"),
            P("fs", "tp"),
            P("fs", "tp"),
        ),
        check_vma=False,
    )
```

```python
import functools
import jax
import jax.numpy as jnp
from jax import lax
from jax.experimental import pallas as pl
from jax.experimental.pallas import tpu as pltpu
from jax.sharding import PartitionSpec as P

AW = 1024
RANK = 128


first_decay = 0.8
second_decay = 0.9
learning_rate = 0.02
norm_epsilon = 1e-06
contract_leading = (((0,), (0,)), ((), ()))


def moments(projected, first_old, second_old, clip_factor):
    scaled = clip_factor * projected
    first_new = first_decay * first_old + (1.0 - first_decay) * scaled
    second_new = second_decay * second_old + (1.0 - second_decay) * scaled * scaled
    return (first_new, second_new, first_new / jnp.sqrt(second_new))


def split_product(reduced, other):
    upper = reduced.astype(jnp.bfloat16)
    lower = (reduced - upper.astype(jnp.float32)).astype(jnp.bfloat16)
    rank_count = reduced.shape[1]
    stacked = jnp.concatenate([upper, lower], axis=1)
    both = lax.dot_general(stacked, other, contract_leading, preferred_element_type=jnp.float32)
    return both[:rank_count] + both[rank_count:]


def local(
    saved_hidden,
    grad_value,
    saved_mixed,
    grad_output,
    basis_value,
    basis_output,
    weight_value,
    weight_output,
    first_value,
    second_value,
    first_output,
    second_output,
):
    row_count = weight_value.shape[0]
    moment_count = first_value.shape[0]
    fs_index = lax.axis_index("fs")
    row_first = fs_index * row_count
    moment_first = fs_index * moment_count
    value_basis_rows = lax.dynamic_slice_in_dim(basis_value, row_first, row_count, 0).astype(
        jnp.float32
    )
    output_basis_rows = lax.dynamic_slice_in_dim(basis_output, row_first, row_count, 0).astype(
        jnp.float32
    )
    reduced_hidden = jnp.dot(saved_hidden, basis_value, preferred_element_type=jnp.float32)
    reduced_output = jnp.dot(grad_output, basis_output, preferred_element_type=jnp.float32)
    part_value = split_product(reduced_hidden, grad_value)
    part_output = split_product(reduced_output, saved_mixed)
    projected_value, projected_output = lax.psum((part_value, part_output), ("fs", "rep"))
    local_squares = jnp.sum(projected_value * projected_value) + jnp.sum(
        projected_output * projected_output
    )
    total_squares = lax.psum(local_squares, "tp")
    mean_square = total_squares / (2 * RANK * AW)
    clip_factor = jnp.minimum(1.0, 1.0 / jnp.sqrt(mean_square + norm_epsilon))
    value_slice = lax.dynamic_slice_in_dim(projected_value, moment_first, moment_count, 0)
    output_slice = lax.dynamic_slice_in_dim(projected_output, moment_first, moment_count, 0)
    new_first_value, new_second_value, value_direction_rows = moments(
        value_slice, first_value, second_value, clip_factor
    )
    new_first_output, new_second_output, output_direction_rows = moments(
        output_slice, first_output, second_output, clip_factor
    )
    direction_value, direction_output = (
        lax.all_gather(value_direction_rows, "fs", axis=0, tiled=True),
        lax.all_gather(output_direction_rows, "fs", axis=0, tiled=True),
    )
    step_value = jnp.dot(value_basis_rows, direction_value, precision=lax.Precision.HIGHEST)
    step_output = jnp.dot(output_basis_rows, direction_output, precision=lax.Precision.HIGHEST).T
    new_weight_value = weight_value - learning_rate * step_value
    new_weight_output = weight_output - learning_rate * step_output
    copy_value, copy_output = (
        lax.all_gather(new_weight_value.astype(jnp.bfloat16), "fs", axis=0, tiled=True),
        lax.all_gather(new_weight_output.astype(jnp.bfloat16), "fs", axis=1, tiled=True),
    )
    return (
        step_value,
        step_output,
        new_weight_value,
        new_weight_output,
        copy_value,
        copy_output,
        new_first_value,
        new_second_value,
        new_first_output,
        new_second_output,
    )


MESH = pl.DeviceIdType.MESH


def remote(src, dst, send, recv, **where):
    return pltpu.make_async_remote_copy(
        src_ref=src, dst_ref=dst, send_sem=send, recv_sem=recv, device_id=where, device_id_type=MESH
    )


def exchange(
    fs_count, rep_count, tp_count,
    hidden, grad_value, mixed, grad_output, basis_value, basis_output, weight_value, weight_output,
    first_value, second_value, first_output, second_output,
    direction, owned, clip, all_value, all_output,
    tokens_in, thin_in, basis_in, value_in, output_in, moment_in,
    part, landed, squares_tp, squares_group,
    load_sem, near_send, near_recv, side_send, side_recv, part_send, part_recv,
    tp_send, tp_recv, group_send, group_recv, owned_send, owned_recv, turn_send, turn_recv,
):
    group = fs_count * rep_count
    fs, rep, tp = lax.axis_index("fs"), lax.axis_index("rep"), lax.axis_index("tp")
    me = fs * rep_count + rep
    tokens = hidden.shape[0]
    rows = part.shape[2]
    width = part.shape[3]
    half = tokens // 2

    loads = []

    def load(source, target):
        copy = pltpu.make_async_copy(source, target, load_sem.at[len(loads)])
        copy.start()
        loads.append(copy)
        return copy

    weight_loads = [load(weight_value, value_in), load(weight_output, output_in)]
    stream_loads = []
    for a, (big, thin, basis) in enumerate(
        ((hidden, grad_value, basis_value), (grad_output, mixed, basis_output))
    ):
        first = load(basis, basis_in.at[a])
        second = load(thin, thin_in.at[a])
        blocks = [
            load(big.at[pl.ds(c * half, half)], tokens_in.at[a, pl.ds(c * half, half)])
            for c in range(2)
        ]
        stream_loads.append((first, second, blocks))
    moment_loads = [
        load(source.at[pl.ds(pl.multiple_of(rep * rows, rows), rows)], moment_in.at[i])
        for i, source in enumerate((first_value, first_output, second_value, second_output))
    ]

    def member(k):
        other = lax.rem(me + k, group)
        return {"fs": other // rep_count, "rep": lax.rem(other, rep_count)}

    barrier = pltpu.get_barrier_semaphore()
    for k in range(1, group):
        pl.semaphore_signal(barrier, inc=1, device_id=member(k), device_id_type=MESH)
    for k in range(1, tp_count):
        pl.semaphore_signal(
            barrier, inc=1, device_id={"tp": lax.rem(tp + k, tp_count)}, device_id_type=MESH
        )
    for copy in weight_loads:
        copy.wait()
    all_value[fs] = value_in[...].astype(jnp.bfloat16)
    all_output[fs] = output_in[...].astype(jnp.bfloat16)
    pl.semaphore_wait(barrier, group - 1 + tp_count - 1)

    share_value = value_in.shape[0] // rep_count
    share_output = output_in.shape[0] // rep_count
    shares = (
        (all_value, pl.ds(pl.multiple_of(rep * share_value, share_value), share_value)),
        (all_output, pl.ds(pl.multiple_of(rep * share_output, share_output), share_output)),
    )
    sent = []

    def send(copy):
        copy.start()
        sent.append(copy)
        return copy

    def hop(a, way, d):
        buffer, rows_here = shares[a]
        step = 1 if way == 0 else -1
        block = buffer.at[fs - step * d, rows_here]
        return remote(
            block, block, near_send.at[a, way, d], near_recv.at[a, way, d], fs=fs + step
        )

    def arrival(a, way, d):
        buffer, rows_here = shares[a]
        step = 1 if way == 0 else -1
        block = buffer.at[fs - step * d, rows_here]
        return remote(
            block, block, near_send.at[a, way, d - 1], near_recv.at[a, way, d - 1], fs=fs - step
        )

    def across(a, way, d, j):
        buffer, rows_here = shares[a]
        step = 1 if way == 0 else -1
        block = buffer.at[fs - step * d, rows_here]
        return remote(
            block, block, side_send.at[a, way, d - 1, j - 1], side_recv.at[a, way, d - 1, j - 1],
            rep=lax.rem(rep + j, rep_count),
        )

    def reaches(way, d):
        return fs >= d if way == 0 else fs + d < fs_count

    def leaves(way, d):
        onward = fs < fs_count - 1 if way == 0 else fs > 0
        return jnp.logical_and(onward, reaches(way, d))

    def send_weights(d):
        for way in range(2):
            @pl.when(leaves(way, d))
            def _():
                for a in range(2):
                    hop(a, way, d).start()

    def pass_weights(d):
        for a in range(2):
            for way in range(2):
                @pl.when(reaches(way, d))
                def _():
                    arrival(a, way, d).wait_recv()

                if d < fs_count - 1:
                    @pl.when(leaves(way, d))
                    def _():
                        hop(a, way, d).start()

                @pl.when(reaches(way, d))
                def _():
                    for j in range(1, rep_count):
                        across(a, way, d, j).start()

    def settle_weights():
        for d in range(fs_count):
            for way in range(2):
                if d < fs_count - 1:
                    @pl.when(leaves(way, d))
                    def _():
                        for a in range(2):
                            hop(a, way, d).wait_send()

                if d > 0:
                    @pl.when(reaches(way, d))
                    def _():
                        for a in range(2):
                            for j in range(1, rep_count):
                                across(a, way, d, j).wait()

    send_weights(0)

    parts = []
    for a in range(2):
        first, second, blocks = stream_loads[a]
        first.wait()
        second.wait()
        total = None
        for c in range(2):
            blocks[c].wait()
            reduced = jnp.dot(
                tokens_in[a, pl.ds(c * half, half)], basis_in[a], preferred_element_type=jnp.float32
            )
            product = split_product(reduced, thin_in[a, pl.ds(c * half, half)])
            total = product if total is None else total + product
        part[a] = total.reshape(group, rows, width)
        for k in range(1, group):
            other = lax.rem(me + k, group)
            parts.append(send(remote(
                part.at[a, other], landed.at[a, k - 1],
                part_send.at[a, k - 1], part_recv.at[a, k - 1], **member(k),
            )))

    for d in range(1, 2):
        pass_weights(d)
    for copy in parts:
        copy.wait_recv()
    squares = jnp.zeros((rows, width), jnp.float32)
    for a in range(2):
        summed = part[a, me]
        for k in range(group - 1):
            summed = summed + landed[a, k]
        owned[rep, a] = summed
        squares = squares + summed * summed
    squares_tp[0] = jnp.full(squares_tp.shape[1:], jnp.sum(squares), jnp.float32)
    tp_copies = [
        send(remote(
            squares_tp.at[0], squares_tp.at[k], tp_send.at[k - 1], tp_recv.at[k - 1],
            tp=lax.rem(tp + k, tp_count),
        ))
        for k in range(1, tp_count)
    ]
    owned_copies = [
        send(remote(
            owned.at[rep], owned.at[rep], owned_send.at[j - 1], owned_recv.at[j - 1],
            rep=lax.rem(rep + j, rep_count),
        ))
        for j in range(1, rep_count)
    ]
    for copy in tp_copies:
        copy.wait_recv()
    squares_group[me] = jnp.sum(squares_tp[...], axis=0)
    group_copies = [
        send(remote(
            squares_group.at[me], squares_group.at[me], group_send.at[k - 1], group_recv.at[k - 1],
            **member(k),
        ))
        for k in range(1, group)
    ]
    for d in range(2, 3):
        pass_weights(d)
    for copy in moment_loads:
        copy.wait()
    for copy in group_copies:
        copy.wait_recv()
    mean_square = jnp.sum(squares_group[...], axis=0) / (2 * RANK * AW)
    factor = jnp.minimum(1.0, 1.0 / jnp.sqrt(mean_square + norm_epsilon))
    clip[...] = factor
    scale = factor[:1, :1]
    for a in range(2):
        _, _, turned = moments(owned[rep, a], moment_in[a], moment_in[2 + a], scale)
        direction[me, a] = turned.astype(jnp.bfloat16)
    turn_copies = [
        send(remote(
            direction.at[me], direction.at[me], turn_send.at[k - 1], turn_recv.at[k - 1], **member(k)
        ))
        for k in range(1, group)
    ]
    for d in range(3, fs_count):
        pass_weights(d)
    for copy in owned_copies + turn_copies:

        copy.wait_recv()
    for copy in sent:
        copy.wait_send()
    settle_weights()


def finish(
    direction, owned, clip, all_value, all_output, basis_value, basis_output,
    weight_value, weight_output, first_value, second_value, first_output, second_output,
    step_value, step_output, new_weight_value, new_weight_output, copy_value, copy_output,
    new_first_value, new_second_value, new_first_output, new_second_output,
):
    fs = lax.axis_index("fs")
    count = weight_value.shape[0]
    width = weight_value.shape[1]
    scale = clip[:1, :1]
    outputs = ((new_first_value, new_second_value), (new_first_output, new_second_output))
    for a, (first, second) in enumerate(
        ((first_value, second_value), (first_output, second_output))
    ):
        projected = owned[:, a].reshape(first.shape)
        new_first, new_second, _ = moments(projected, first[...], second[...], scale)
        outputs[a][0][...] = new_first
        outputs[a][1][...] = new_second
    turn_value = direction[:, 0].reshape(RANK, width)
    turn_output = direction[:, 1].reshape(RANK, width).astype(jnp.float32).T.astype(jnp.bfloat16)
    across = (((1,), (1,)), ((), ()))

    def value_step(rows_here):
        return jnp.dot(basis_value[rows_here], turn_value, preferred_element_type=jnp.float32)

    def output_step(rows_here):
        return lax.dot_general(
            turn_output, basis_output[rows_here], across, preferred_element_type=jnp.float32
        )

    mine = pl.ds(pl.multiple_of(fs * count, count), count)
    step = value_step(mine)
    step_value[...] = step
    new_weight_value[...] = weight_value[...] - learning_rate * step
    step = output_step(mine)
    step_output[...] = step
    new_weight_output[...] = weight_output[...] - learning_rate * step
    for f in range(all_value.shape[0]):
        here = pl.ds(f * count, count)
        copy_value[here] = (
            all_value[f].astype(jnp.float32) - learning_rate * value_step(here)
        ).astype(jnp.bfloat16)
        copy_output[:, here] = (
            all_output[f].astype(jnp.float32) - learning_rate * output_step(here)
        ).astype(jnp.bfloat16)


def kernels(
    fs_count, rep_count, tp_count,
    saved_hidden, grad_value, saved_mixed, grad_output, basis_value, basis_output,
    weight_value, weight_output, first_value, second_value, first_output, second_output,
):
    group = fs_count * rep_count
    tokens, model = saved_hidden.shape
    count, width = weight_value.shape
    rank = basis_value.shape[1]
    rows = rank // group
    f32, bf16 = jnp.float32, jnp.bfloat16
    shape = jax.ShapeDtypeStruct
    dma = pltpu.SemaphoreType.DMA
    anywhere = pl.BlockSpec(memory_space=pl.ANY)
    in_vmem = pl.BlockSpec(memory_space=pltpu.VMEM)
    direction, owned, clip, all_value, all_output = pl.pallas_call(
        functools.partial(exchange, fs_count, rep_count, tp_count),
        out_shape=(
            shape((group, 2, rows, width), bf16),
            shape((rep_count, 2, rows, width), f32),
            shape((8, 128), f32),
            shape((fs_count, count, width), bf16),
            shape((fs_count, width, count), bf16),
        ),
        in_specs=[anywhere] * 12,
        out_specs=(in_vmem,) * 5,
        scratch_shapes=[
            pltpu.VMEM((2, tokens, model), bf16),
            pltpu.VMEM((2, tokens, width), bf16),
            pltpu.VMEM((2, model, rank), bf16),
            pltpu.VMEM((count, width), f32),
            pltpu.VMEM((width, count), f32),
            pltpu.VMEM((4, rows, width), f32),
            pltpu.VMEM((2, group, rows, width), f32),
            pltpu.VMEM((2, group - 1, rows, width), f32),
            pltpu.VMEM((tp_count, 8, 128), f32),
            pltpu.VMEM((group, 8, 128), f32),
            dma((14,)),
            dma((2, 2, fs_count - 1)), dma((2, 2, fs_count - 1)),
            dma((2, 2, fs_count - 1, rep_count - 1)), dma((2, 2, fs_count - 1, rep_count - 1)),
            dma((2, group - 1)), dma((2, group - 1)),
            dma((tp_count - 1,)), dma((tp_count - 1,)),
            dma((group - 1,)), dma((group - 1,)),
            dma((rep_count - 1,)), dma((rep_count - 1,)),
            dma((group - 1,)), dma((group - 1,)),
        ],
        compiler_params=pltpu.CompilerParams(
            collective_id=0, has_side_effects=True, vmem_limit_bytes=60 * 1024 * 1024
        ),
        name="exchange",
    )(
        saved_hidden, grad_value, saved_mixed, grad_output, basis_value, basis_output,
        weight_value, weight_output, first_value, second_value, first_output, second_output,
    )
    moment = shape(first_value.shape, f32)
    return pl.pallas_call(
        finish,
        out_shape=(
            shape((count, width), f32), shape((width, count), f32),
            shape((count, width), f32), shape((width, count), f32),
            shape((model, width), bf16), shape((width, model), bf16),
            moment, moment, moment, moment,
        ),
        in_specs=[in_vmem] * 13,
        out_specs=(in_vmem,) * 10,
        compiler_params=pltpu.CompilerParams(vmem_limit_bytes=60 * 1024 * 1024),
        name="finish",
    )(
        direction, owned, clip, all_value, all_output, basis_value, basis_output,
        weight_value, weight_output, first_value, second_value, first_output, second_output,
    )


def solution(mesh):
    fs_count, rep_count, tp_count = mesh.shape["fs"], mesh.shape["rep"], mesh.shape["tp"]
    whole_tiles = RANK % (16 * fs_count * rep_count) == 0
    body = functools.partial(kernels, fs_count, rep_count, tp_count) if whole_tiles else local
    return jax.shard_map(
        body,
        mesh=mesh,
        in_specs=(
            P(("fs", "rep"), None),
            P(("fs", "rep"), "tp"),
            P(("fs", "rep"), "tp"),
            P(("fs", "rep"), None),
            P(),
            P(),
            P("fs", "tp"),
            P("tp", "fs"),
            P("fs", "tp"),
            P("fs", "tp"),
            P("fs", "tp"),
            P("fs", "tp"),
        ),
        out_specs=(
            P("fs", "tp"),
            P("tp", "fs"),
            P("fs", "tp"),
            P("tp", "fs"),
            P(None, "tp"),
            P("tp", None),
            P("fs", "tp"),
            P("fs", "tp"),
            P("fs", "tp"),
            P("fs", "tp"),
        ),
        check_vma=False,
    )
```

```python
import functools
import jax
import jax.numpy as jnp
from jax import lax
from jax.experimental import pallas as pl
from jax.experimental.pallas import tpu as pltpu
from jax.sharding import PartitionSpec as P

AW = 1024
RANK = 128


first_decay = 0.8
second_decay = 0.9
learning_rate = 0.02
norm_epsilon = 1e-06
contract_leading = (((0,), (0,)), ((), ()))


def moments(projected, first_old, second_old, clip_factor):
    scaled = clip_factor * projected
    first_new = first_decay * first_old + (1.0 - first_decay) * scaled
    second_new = second_decay * second_old + (1.0 - second_decay) * scaled * scaled
    return (first_new, second_new, first_new / jnp.sqrt(second_new))


def split_product(reduced, other):
    upper = reduced.astype(jnp.bfloat16)
    lower = (reduced - upper.astype(jnp.float32)).astype(jnp.bfloat16)
    rank_count = reduced.shape[1]
    stacked = jnp.concatenate([upper, lower], axis=1)
    both = lax.dot_general(stacked, other, contract_leading, preferred_element_type=jnp.float32)
    return both[:rank_count] + both[rank_count:]


def local(
    saved_hidden,
    grad_value,
    saved_mixed,
    grad_output,
    basis_value,
    basis_output,
    weight_value,
    weight_output,
    first_value,
    second_value,
    first_output,
    second_output,
):
    row_count = weight_value.shape[0]
    moment_count = first_value.shape[0]
    fs_index = lax.axis_index("fs")
    row_first = fs_index * row_count
    moment_first = fs_index * moment_count
    value_basis_rows = lax.dynamic_slice_in_dim(basis_value, row_first, row_count, 0).astype(
        jnp.float32
    )
    output_basis_rows = lax.dynamic_slice_in_dim(basis_output, row_first, row_count, 0).astype(
        jnp.float32
    )
    reduced_hidden = jnp.dot(saved_hidden, basis_value, preferred_element_type=jnp.float32)
    reduced_output = jnp.dot(grad_output, basis_output, preferred_element_type=jnp.float32)
    part_value = split_product(reduced_hidden, grad_value)
    part_output = split_product(reduced_output, saved_mixed)
    projected_value, projected_output = lax.psum((part_value, part_output), ("fs", "rep"))
    local_squares = jnp.sum(projected_value * projected_value) + jnp.sum(
        projected_output * projected_output
    )
    total_squares = lax.psum(local_squares, "tp")
    mean_square = total_squares / (2 * RANK * AW)
    clip_factor = jnp.minimum(1.0, 1.0 / jnp.sqrt(mean_square + norm_epsilon))
    value_slice = lax.dynamic_slice_in_dim(projected_value, moment_first, moment_count, 0)
    output_slice = lax.dynamic_slice_in_dim(projected_output, moment_first, moment_count, 0)
    new_first_value, new_second_value, value_direction_rows = moments(
        value_slice, first_value, second_value, clip_factor
    )
    new_first_output, new_second_output, output_direction_rows = moments(
        output_slice, first_output, second_output, clip_factor
    )
    direction_value, direction_output = (
        lax.all_gather(value_direction_rows, "fs", axis=0, tiled=True),
        lax.all_gather(output_direction_rows, "fs", axis=0, tiled=True),
    )
    step_value = jnp.dot(value_basis_rows, direction_value, precision=lax.Precision.HIGHEST)
    step_output = jnp.dot(output_basis_rows, direction_output, precision=lax.Precision.HIGHEST).T
    new_weight_value = weight_value - learning_rate * step_value
    new_weight_output = weight_output - learning_rate * step_output
    copy_value, copy_output = (
        lax.all_gather(new_weight_value.astype(jnp.bfloat16), "fs", axis=0, tiled=True),
        lax.all_gather(new_weight_output.astype(jnp.bfloat16), "fs", axis=1, tiled=True),
    )
    return (
        step_value,
        step_output,
        new_weight_value,
        new_weight_output,
        copy_value,
        copy_output,
        new_first_value,
        new_second_value,
        new_first_output,
        new_second_output,
    )


MESH = pl.DeviceIdType.MESH


def remote(src, dst, send, recv, **where):
    return pltpu.make_async_remote_copy(
        src_ref=src, dst_ref=dst, send_sem=send, recv_sem=recv, device_id=where, device_id_type=MESH
    )


def exchange(
    fs_count, rep_count, tp_count,
    hidden, grad_value, mixed, grad_output, basis_value, basis_output, weight_value, weight_output,
    first_value, second_value, first_output, second_output,
    direction, owned, clip, all_value, all_output,
    tokens_in, thin_in, basis_in, value_in, output_in, moment_in,
    part, landed, squares_all,
    load_sem, near_send, near_recv, side_send, side_recv, part_send, part_recv,
    square_send, square_recv, owned_send, owned_recv, turn_send, turn_recv,
):
    group = fs_count * rep_count
    fs, rep, tp = lax.axis_index("fs"), lax.axis_index("rep"), lax.axis_index("tp")
    me = fs * rep_count + rep
    tokens = hidden.shape[0]
    rows = part.shape[2]
    width = part.shape[3]
    half = tokens // 2

    loads = []

    def load(source, target):
        copy = pltpu.make_async_copy(source, target, load_sem.at[len(loads)])
        copy.start()
        loads.append(copy)
        return copy

    weight_loads = [load(weight_value, value_in), load(weight_output, output_in)]
    stream_loads = []
    for a, (big, thin, basis) in enumerate(
        ((hidden, grad_value, basis_value), (grad_output, mixed, basis_output))
    ):
        first = load(basis, basis_in.at[a])
        second = load(thin, thin_in.at[a])
        blocks = [
            load(big.at[pl.ds(c * half, half)], tokens_in.at[a, pl.ds(c * half, half)])
            for c in range(2)
        ]
        stream_loads.append((first, second, blocks))
    moment_loads = [
        load(source.at[pl.ds(pl.multiple_of(rep * rows, rows), rows)], moment_in.at[i])
        for i, source in enumerate((first_value, first_output, second_value, second_output))
    ]

    def member(k):
        other = lax.rem(me + k, group)
        return {"fs": other // rep_count, "rep": lax.rem(other, rep_count)}

    barrier = pltpu.get_barrier_semaphore()
    everyone = group * tp_count

    def anyone(k):
        other = lax.rem(me * tp_count + tp + k, everyone)
        place = other // tp_count
        return {
            "fs": place // rep_count, "rep": lax.rem(place, rep_count), "tp": lax.rem(other, tp_count)
        }

    for k in range(1, everyone):
        pl.semaphore_signal(barrier, inc=1, device_id=anyone(k), device_id_type=MESH)
    for copy in weight_loads:
        copy.wait()
    all_value[fs] = value_in[...].astype(jnp.bfloat16)
    all_output[fs] = output_in[...].astype(jnp.bfloat16)
    pl.semaphore_wait(barrier, everyone - 1)

    share_value = value_in.shape[0] // rep_count
    share_output = output_in.shape[0] // rep_count
    shares = (
        (all_value, pl.ds(pl.multiple_of(rep * share_value, share_value), share_value)),
        (all_output, pl.ds(pl.multiple_of(rep * share_output, share_output), share_output)),
    )
    sent = []

    def send(copy):
        copy.start()
        sent.append(copy)
        return copy

    def hop(a, way, d):
        buffer, rows_here = shares[a]
        step = 1 if way == 0 else -1
        block = buffer.at[fs - step * d, rows_here]
        return remote(
            block, block, near_send.at[a, way, d], near_recv.at[a, way, d], fs=fs + step
        )

    def arrival(a, way, d):
        buffer, rows_here = shares[a]
        step = 1 if way == 0 else -1
        block = buffer.at[fs - step * d, rows_here]
        return remote(
            block, block, near_send.at[a, way, d - 1], near_recv.at[a, way, d - 1], fs=fs - step
        )

    def across(a, way, d, j):
        buffer, rows_here = shares[a]
        step = 1 if way == 0 else -1
        block = buffer.at[fs - step * d, rows_here]
        return remote(
            block, block, side_send.at[a, way, d - 1, j - 1], side_recv.at[a, way, d - 1, j - 1],
            rep=lax.rem(rep + j, rep_count),
        )

    def reaches(way, d):
        return fs >= d if way == 0 else fs + d < fs_count

    def leaves(way, d):
        onward = fs < fs_count - 1 if way == 0 else fs > 0
        return jnp.logical_and(onward, reaches(way, d))

    def send_weights(d):
        for way in range(2):
            @pl.when(leaves(way, d))
            def _():
                for a in range(2):
                    hop(a, way, d).start()

    def pass_weights(d):
        for a in range(2):
            for way in range(2):
                @pl.when(reaches(way, d))
                def _():
                    arrival(a, way, d).wait_recv()

                if d < fs_count - 1:
                    @pl.when(leaves(way, d))
                    def _():
                        hop(a, way, d).start()

                @pl.when(reaches(way, d))
                def _():
                    for j in range(1, rep_count):
                        across(a, way, d, j).start()

    def settle_weights():
        for d in range(fs_count):
            for way in range(2):
                if d < fs_count - 1:
                    @pl.when(leaves(way, d))
                    def _():
                        for a in range(2):
                            hop(a, way, d).wait_send()

                if d > 0:
                    @pl.when(reaches(way, d))
                    def _():
                        for a in range(2):
                            for j in range(1, rep_count):
                                across(a, way, d, j).wait()

    send_weights(0)

    parts = []
    for a in range(2):
        first, second, blocks = stream_loads[a]
        first.wait()
        second.wait()
        total = None
        for c in range(2):
            blocks[c].wait()
            reduced = jnp.dot(
                tokens_in[a, pl.ds(c * half, half)], basis_in[a], preferred_element_type=jnp.float32
            )
            product = split_product(reduced, thin_in[a, pl.ds(c * half, half)])
            total = product if total is None else total + product
        part[a] = total.reshape(group, rows, width)
        for k in range(1, group):
            other = lax.rem(me + k, group)
            parts.append(send(remote(
                part.at[a, other], landed.at[a, k - 1],
                part_send.at[a, k - 1], part_recv.at[a, k - 1], **member(k),
            )))

    for d in range(1, 2):
        pass_weights(d)
    for copy in parts:
        copy.wait_recv()
    squares = jnp.zeros((rows, width), jnp.float32)
    for a in range(2):
        summed = part[a, me]
        for k in range(group - 1):
            summed = summed + landed[a, k]
        owned[rep, a] = summed
        squares = squares + summed * summed
    place = me * tp_count + tp
    squares_all[place] = jnp.full(squares_all.shape[1:], jnp.sum(squares), jnp.float32)
    square_copies = [
        send(remote(
            squares_all.at[place], squares_all.at[place],
            square_send.at[k - 1], square_recv.at[k - 1], **anyone(k),
        ))
        for k in range(1, everyone)
    ]
    owned_copies = [
        send(remote(
            owned.at[rep], owned.at[rep], owned_send.at[j - 1], owned_recv.at[j - 1],
            rep=lax.rem(rep + j, rep_count),
        ))
        for j in range(1, rep_count)
    ]
    for d in range(2, 3):
        pass_weights(d)
    for copy in moment_loads:
        copy.wait()
    for copy in square_copies:
        copy.wait_recv()
    mean_square = jnp.sum(squares_all[...], axis=0) / (2 * RANK * AW)
    factor = jnp.minimum(1.0, 1.0 / jnp.sqrt(mean_square + norm_epsilon))
    clip[...] = jnp.broadcast_to(factor, clip.shape)
    scale = factor[:1, :1]
    for a in range(2):
        _, _, turned = moments(owned[rep, a], moment_in[a], moment_in[2 + a], scale)
        direction[me, a] = turned.astype(jnp.bfloat16)
    turn_copies = [
        send(remote(
            direction.at[me], direction.at[me], turn_send.at[k - 1], turn_recv.at[k - 1], **member(k)
        ))
        for k in range(1, group)
    ]
    for d in range(3, fs_count):
        pass_weights(d)
    for copy in owned_copies + turn_copies:

        copy.wait_recv()
    for copy in sent:
        copy.wait_send()
    settle_weights()


def finish(*refs):
    sources, targets, inside, made = refs[:13], refs[13:23], refs[23:36], refs[36:46]
    load_sem, store_sem = refs[46:]
    (
        direction, owned, clip, all_value, all_output, basis_value, basis_output,
        weight_value, weight_output, first_value, second_value, first_output, second_output,
    ) = inside
    fs_count = all_value.shape[0]
    fs = lax.axis_index("fs")
    count = weight_value.shape[0]
    width = weight_value.shape[1]
    loads = [
        pltpu.make_async_copy(sources[i], inside[i], load_sem.at[i]) for i in range(len(inside))
    ]
    for i in (0, 5, 7, 6, 8, 3, 4, 1, 2, 9, 10, 11, 12):
        loads[i].start()
    stores = []

    def store(i, here=None):
        source, target = made[i], targets[i]
        if here is not None:
            source, target = source.at[here], target.at[here]
        copy = pltpu.make_async_copy(source, target, store_sem.at[len(stores)])
        copy.start()
        stores.append(copy)

    def ready(*which):
        for i in which:
            loads[i].wait()

    across = (((1,), (1,)), ((), ()))
    mine = pl.ds(pl.multiple_of(fs * count, count), count)
    ready(0, 5)
    turn_value = direction[:, 0].reshape(RANK, width)
    turn_output = direction[:, 1].reshape(RANK, width).astype(jnp.float32).T.astype(jnp.bfloat16)

    def value_step(rows_here):
        return jnp.dot(basis_value[rows_here], turn_value, preferred_element_type=jnp.float32)

    def output_step(rows_here):
        return lax.dot_general(
            turn_output, basis_output[rows_here], across, preferred_element_type=jnp.float32
        )

    step = value_step(mine)
    made[0][...] = step
    store(0)
    ready(7)
    made[2][...] = weight_value[...] - learning_rate * step
    store(2)
    ready(6)
    step = output_step(mine)
    made[1][...] = step
    store(1)
    ready(8)
    made[3][...] = weight_output[...] - learning_rate * step
    store(3)
    ready(3)
    for f in range(fs_count):
        here = pl.ds(f * count, count)
        made[4][here] = (
            all_value[f].astype(jnp.float32) - learning_rate * value_step(here)
        ).astype(jnp.bfloat16)
        store(4, here)
    ready(4)
    for f in range(fs_count):
        here = pl.ds(f * count, count)
        made[5][:, here] = (
            all_output[f].astype(jnp.float32) - learning_rate * output_step(here)
        ).astype(jnp.bfloat16)
        store(5, (slice(None), here))
    ready(1, 2, 9, 10, 11, 12)
    scale = clip[:1, :1]
    for a, (first, second) in enumerate(
        ((first_value, second_value), (first_output, second_output))
    ):
        projected = owned[:, a].reshape(first.shape)
        new_first, new_second, _ = moments(projected, first[...], second[...], scale)
        made[6 + 2 * a][...] = new_first
        made[7 + 2 * a][...] = new_second
        store(6 + 2 * a)
        store(7 + 2 * a)
    for copy in stores:
        copy.wait()


def kernels(
    fs_count, rep_count, tp_count,
    saved_hidden, grad_value, saved_mixed, grad_output, basis_value, basis_output,
    weight_value, weight_output, first_value, second_value, first_output, second_output,
):
    group = fs_count * rep_count
    tokens, model = saved_hidden.shape
    count, width = weight_value.shape
    rank = basis_value.shape[1]
    rows = rank // group
    f32, bf16 = jnp.float32, jnp.bfloat16
    shape = jax.ShapeDtypeStruct
    dma = pltpu.SemaphoreType.DMA
    anywhere = pl.BlockSpec(memory_space=pl.ANY)
    in_vmem = pl.BlockSpec(memory_space=pltpu.VMEM)
    direction, owned, clip, all_value, all_output = pl.pallas_call(
        functools.partial(exchange, fs_count, rep_count, tp_count),
        out_shape=(
            shape((group, 2, rows, width), bf16),
            shape((rep_count, 2, rows, width), f32),
            shape((8, 128), f32),
            shape((fs_count, count, width), bf16),
            shape((fs_count, width, count), bf16),
        ),
        in_specs=[anywhere] * 12,
        out_specs=(in_vmem,) * 5,
        scratch_shapes=[
            pltpu.VMEM((2, tokens, model), bf16),
            pltpu.VMEM((2, tokens, width), bf16),
            pltpu.VMEM((2, model, rank), bf16),
            pltpu.VMEM((count, width), f32),
            pltpu.VMEM((width, count), f32),
            pltpu.VMEM((4, rows, width), f32),
            pltpu.VMEM((2, group, rows, width), f32),
            pltpu.VMEM((2, group - 1, rows, width), f32),
            pltpu.VMEM((group * tp_count, 1, 128), f32),
            dma((14,)),
            dma((2, 2, fs_count - 1)), dma((2, 2, fs_count - 1)),
            dma((2, 2, fs_count - 1, rep_count - 1)), dma((2, 2, fs_count - 1, rep_count - 1)),
            dma((2, group - 1)), dma((2, group - 1)),
            dma((group * tp_count - 1,)), dma((group * tp_count - 1,)),
            dma((rep_count - 1,)), dma((rep_count - 1,)),
            dma((group - 1,)), dma((group - 1,)),
        ],
        compiler_params=pltpu.CompilerParams(
            collective_id=0, has_side_effects=True, vmem_limit_bytes=60 * 1024 * 1024
        ),
        name="exchange",
    )(
        saved_hidden, grad_value, saved_mixed, grad_output, basis_value, basis_output,
        weight_value, weight_output, first_value, second_value, first_output, second_output,
    )
    moment = shape(first_value.shape, f32)
    operands = (
        direction, owned, clip, all_value, all_output, basis_value, basis_output,
        weight_value, weight_output, first_value, second_value, first_output, second_output,
    )
    results = (
        shape((count, width), f32), shape((width, count), f32),
        shape((count, width), f32), shape((width, count), f32),
        shape((model, width), bf16), shape((width, model), bf16),
        moment, moment, moment, moment,
    )
    return pl.pallas_call(
        finish,
        out_shape=results,
        in_specs=[anywhere] * len(operands),
        out_specs=(anywhere,) * len(results),
        scratch_shapes=[pltpu.VMEM(x.shape, x.dtype) for x in operands + results]
        + [dma((len(operands),)), dma((len(results) - 2 + 2 * fs_count,))],
        compiler_params=pltpu.CompilerParams(vmem_limit_bytes=60 * 1024 * 1024),
        name="finish",
    )(*operands)


def solution(mesh):
    fs_count, rep_count, tp_count = mesh.shape["fs"], mesh.shape["rep"], mesh.shape["tp"]
    whole_tiles = RANK % (16 * fs_count * rep_count) == 0
    body = functools.partial(kernels, fs_count, rep_count, tp_count) if whole_tiles else local
    return jax.shard_map(
        body,
        mesh=mesh,
        in_specs=(
            P(("fs", "rep"), None),
            P(("fs", "rep"), "tp"),
            P(("fs", "rep"), "tp"),
            P(("fs", "rep"), None),
            P(),
            P(),
            P("fs", "tp"),
            P("tp", "fs"),
            P("fs", "tp"),
            P("fs", "tp"),
            P("fs", "tp"),
            P("fs", "tp"),
        ),
        out_specs=(
            P("fs", "tp"),
            P("tp", "fs"),
            P("fs", "tp"),
            P("tp", "fs"),
            P(None, "tp"),
            P("tp", None),
            P("fs", "tp"),
            P("fs", "tp"),
            P("fs", "tp"),
            P("fs", "tp"),
        ),
        check_vma=False,
    )
```
